32 devices in a mesh: st: 8 (over z, y), tp: 4 (over x, core).
Axes of the slice: x: 2, y: 2, z: 4, core: 2. Of those that a mesh axis runs over, the one named last changes fastest.
Arguments:
- tokens: bfloat16 [3072, 2048], P('st', 'tp'), may hold values from -6 to 6
- cotangent: bfloat16 [3072, 1024], P('st', 'tp'), may hold values from -48 to 48
- mix_query: bfloat16 [3072, 1024], P('st', 'tp'), may hold values from -6 to 6
- mix_key: bfloat16 [3072, 1024], P('st', 'tp'), may hold values from -6 to 6
- mix_value: bfloat16 [3072, 1024], P('st', 'tp'), may hold values from -24 to 24
- beta_pre: float32 [8, 3072], P('tp', 'st'), may hold values from -9 to 9
- decay_pre: float32 [8, 3072], P('tp', 'st'), may hold values from -8 to 6
- decay_rate: float32 [8], P('tp'), may hold values from 0.001 to 0.06
- passages: bfloat16 [128, 64, 2048], P('st'), may hold values from -6 to 6
- passage_ids: int32 [48, 4], P('st'), may hold values from 0 to 127, as said below
- query_weight: bfloat16 [2048, 1024], P(None, 'tp'), may hold values from -0.125 to 0.125
- key_weight: bfloat16 [2048, 1024], P(None, 'tp'), may hold values from -0.125 to 0.125
- value_weight: bfloat16 [2048, 1024], P(None, 'tp'), may hold values from -0.125 to 0.125
- gate_weight: bfloat16 [4, 2048], P('tp'), may hold values from -0.125 to 0.125
Outputs:
- token_grad: bfloat16 [3072, 2048], P('st', 'tp')
- passage_grad: bfloat16 [128, 64, 2048], P('st', None, 'tp')
- key_weight_grad: float32 [2048, 1024], P('st', 'tp')
The draws below stay inside these ranges and needn't reach their ends.
Inputs may be any that keep to these rules, and one draw needn't show every extreme that they name: Passage p is stored on index p // 16 of st. The rows of passage_ids read by one index of st name at most 3 passages stored on any one index of st, and exactly 3 on some.
All inputs are finite; a program needn't handle non-finite values.
Results may differ from the reference program's by a relative error of at most 0.012.
The reference program's roundings to bfloat16 on the way count: a program that leaves them out, or rounds other values in their place, can miss the bound.
Values may be sent and summed in bfloat16 or wider, within the bound.
A program may use at most 128 MiB of HBM per device.

```python
import math
import jax
import jax.numpy as jnp
from jax import lax

D = 2048
HEADS = 4
HEAD = 256
MIX_HEADS = 8
MIX_DIM = 128
SPAN = 64
BLOCK = 64
PER_BLOCK = 4
PROWS = 64
TOK_DEV = 384
PASS_DEV = 16
TOKENS = 3072
BLOCKS = 48
REQ_DEV = 24
CAP = 3
PASSAGES = 128
N_ST = 8


def draw_passage_ids(key, part):
    slot_count = N_ST * CAP
    shift_table = jax.random.randint(jax.random.fold_in(key, 9001), (N_ST,), 0, PASS_DEV)

    def per_reader(reader_idx):
        keys_split = jax.random.split(jax.random.fold_in(key, reader_idx), 4)
        rank_score = jax.random.permutation(keys_split[0], slot_count).astype(jnp.int32)
        slot_owner = jnp.arange(slot_count, dtype=jnp.int32) // CAP
        forced = (slot_owner == (reader_idx - 1) % N_ST) | (slot_owner == (reader_idx + N_ST // 2) % N_ST)
        rank_score = rank_score + forced.astype(jnp.int32) * (2 * slot_count)
        _, chosen = lax.top_k(rank_score, REQ_DEV)
        chosen = chosen.astype(jnp.int32)[jax.random.permutation(keys_split[1], REQ_DEV)]
        owner_ids = chosen // CAP
        first_draw = jax.random.randint(keys_split[2], (REQ_DEV,), 0, PASS_DEV)
        second_draw = jax.random.randint(keys_split[3], (REQ_DEV,), 0, PASS_DEV)
        local_ids = (jnp.minimum(first_draw, second_draw) + shift_table[owner_ids]) % PASS_DEV
        return (owner_ids * PASS_DEV + local_ids).astype(jnp.int32)
    every_id = jax.vmap(per_reader)(jnp.arange(N_ST, dtype=jnp.int32))
    return every_id.reshape(BLOCKS, PER_BLOCK)


def draw_decay_pre(key, part):
    keys_split = jax.random.split(key, 3)
    noise_part = 0.7 * jax.random.normal(keys_split[0], (MIX_HEADS, TOKENS), jnp.float32)
    slow_part = jax.random.uniform(keys_split[1], (MIX_HEADS, TOKENS // SPAN), jnp.float32, -1.2, 1.2)
    device_part = jax.random.uniform(keys_split[2], (MIX_HEADS, N_ST), jnp.float32, -1.0, 1.0)
    values_out = noise_part + jnp.repeat(slow_part, SPAN, axis=1) + jnp.repeat(device_part, TOK_DEV, axis=1)
    return jnp.clip(values_out, -8.0, 6.0)


def spiked(array, rng, source, target, parts, factor):
    owner, partner = [(jnp.arange(array.shape[dim]) // (array.shape[dim] // parts)).reshape([-1 if axis == dim else 1 for axis in range(array.ndim)]) for dim in (source, target)]
    chosen = jax.random.permutation(rng, parts)[partner]
    strong = (owner == chosen) | (owner == (partner + parts // 2) % parts)
    return jnp.where(strong, factor * array, array)


def level_of(key, extent, cuts, low, largest):
    def one(axis_at, blocks):
        draws = jax.random.uniform(jax.random.fold_in(jax.random.fold_in(key, 6), axis_at), (blocks,), jnp.float32, low / len(cuts), largest / len(cuts))
        return jnp.repeat(jnp.exp(draws), extent[axis_at] // blocks).reshape((-1,) + (1,) * (len(extent) - axis_at - 1))

    level = one(*cuts[0])
    for cut in cuts[1:]:
        level = level * one(*cut)
    return level


def scatter_about(rng, shape, scale, reach, pieces=(), kind=jnp.bfloat16):
    loudness = level_of(rng, shape, pieces, -0.22, 0.18) if pieces else 1.0
    values = jax.random.normal(rng, shape, jnp.float32) * scale * loudness
    return jnp.minimum(jnp.maximum(values, -reach), reach).astype(kind)


def noise_with(rng, extent, deviation, most, cuts, heavy, kind=jnp.bfloat16):
    entries = deviation * jax.random.normal(rng, extent, jnp.float32)
    if cuts:
        entries = entries * level_of(rng, extent, cuts, -0.22, 0.18)
    return jnp.clip(spiked(entries, jax.random.fold_in(rng, 3), *heavy), -most, most).astype(kind)


def setup_inputs(seed: int = 0) -> dict:
    streams_of = jax.random.split(jax.random.key(seed), 15)
    tokens = scatter_about(streams_of[0], (TOKENS, D), 1.0, 6.0, ((0, 8), (1, 4)))
    cotangent = scatter_about(streams_of[1], (TOKENS, HEADS * HEAD), 8.0, 48.0, ((0, 8), (1, 4)))
    mix_query = scatter_about(streams_of[2], (TOKENS, MIX_HEADS * MIX_DIM), 1.0, 6.0, ((0, 8), (1, 4)))
    mix_key = scatter_about(streams_of[3], (TOKENS, MIX_HEADS * MIX_DIM), 1.0, 6.0, ((0, 8), (1, 4)))
    mix_value = scatter_about(streams_of[4], (TOKENS, MIX_HEADS * MIX_DIM), 4.0, 24.0, ((0, 8), (1, 4)))
    beta_pre = scatter_about(streams_of[5], (MIX_HEADS, TOKENS), 1.5, 9.0, ((0, 4), (1, 8)), jnp.float32)
    decay_pre = draw_decay_pre(jax.random.fold_in(streams_of[14], 71), 0)
    decay_rate = jnp.clip(jnp.exp(math.log(0.06) - 4.0943445 * jax.random.uniform(streams_of[7], (MIX_HEADS,), jnp.float32) ** level_of(streams_of[7], (MIX_HEADS,), ((0, 4),), -0.2, 0.2)), 0.001, 0.06)
    passages = noise_with(streams_of[8], (PASSAGES, PROWS, D), 1.0, 6.0, ((0, 8),), (0, 2, 8, 2.0))
    passage_ids = draw_passage_ids(jax.random.fold_in(streams_of[14], 71), 0)
    query_weight = scatter_about(streams_of[10], (D, HEADS * HEAD), D ** -0.5, 0.125, ((1, 4),))
    key_weight = scatter_about(streams_of[11], (D, HEADS * HEAD), D ** -0.5, 0.125, ((1, 4),))
    value_weight = scatter_about(streams_of[12], (D, HEADS * HEAD), D ** -0.5, 0.125, ((1, 4),))
    gate_weight = scatter_about(streams_of[13], (HEADS, D), D ** -0.5, 0.125, ((0, 4),))
    return dict(tokens=tokens, cotangent=cotangent, mix_query=mix_query, mix_key=mix_key, mix_value=mix_value, beta_pre=beta_pre, decay_pre=decay_pre, decay_rate=decay_rate, passages=passages, passage_ids=passage_ids, query_weight=query_weight, key_weight=key_weight, value_weight=value_weight, gate_weight=gate_weight)


NORM_FLOOR = 1.0
SCORE_GAIN = 4.0
HIGHEST = lax.Precision.HIGHEST

def to_low(value):
    return lax.optimization_barrier(value.astype(jnp.bfloat16))

def neumann_inverse(strict_part):
    span_size = strict_part.shape[-1]
    unit_eye = jnp.eye(span_size, dtype=jnp.float32)
    running = unit_eye - strict_part
    power_term = strict_part
    for _ in range(span_size.bit_length() - 2):
        power_term = jnp.einsum('...ij,...jk->...ik', power_term, power_term, precision=HIGHEST)
        running = jnp.einsum('...ij,...jk->...ik', running, unit_eye + power_term, precision=HIGHEST)
    return running

def delta_mixer(queries, keys_in, values_in, strength, log_decay):
    heads_n, length, key_dim = queries.shape
    blocks_n = length // SPAN

    def to_blocks(tensor):
        return tensor.reshape(heads_n, blocks_n, SPAN, *tensor.shape[2:])
    queries, keys_in, values_in = (to_blocks(queries), to_blocks(keys_in), to_blocks(values_in))
    strength, log_decay = (to_blocks(strength), to_blocks(log_decay))
    cumulative = jnp.cumsum(log_decay, axis=-1)
    position = jnp.arange(SPAN)
    inclusive = position[:, None] >= position[None, :]
    strictly = position[:, None] > position[None, :]
    spread = jnp.where(inclusive, cumulative[..., :, None] - cumulative[..., None, :], -jnp.inf)
    decay_map = jnp.exp(spread)
    key_gram = jnp.einsum('hncd,hnmd->hncm', keys_in, keys_in, precision=HIGHEST)
    strict_part = jnp.where(strictly, strength[..., :, None] * key_gram * decay_map, 0.0)
    inverse = neumann_inverse(strict_part)
    fresh_vals = jnp.einsum('hncm,hnme->hnce', inverse, values_in * strength[..., None], precision=HIGHEST)
    correction = jnp.einsum('hncm,hnmd->hncd', inverse, keys_in * (strength * jnp.exp(cumulative))[..., None], precision=HIGHEST)
    attend_map = jnp.where(inclusive, jnp.einsum('hncd,hnmd->hncm', queries, keys_in, precision=HIGHEST) * decay_map, 0.0)
    query_dec = queries * jnp.exp(cumulative)[..., None]
    key_dec = keys_in * jnp.exp(cumulative[..., -1:] - cumulative)[..., None]
    carry_decay = jnp.exp(cumulative[..., -1])

    def advance(memory_state, inputs):
        fresh_blk, correct_blk, attend_blk, query_blk, key_blk, decay_blk = inputs
        new_values = fresh_blk - jnp.einsum('hcd,hde->hce', correct_blk, memory_state, precision=HIGHEST)
        output = jnp.einsum('hcd,hde->hce', query_blk, memory_state, precision=HIGHEST) + jnp.einsum('hcm,hme->hce', attend_blk, new_values, precision=HIGHEST)
        memory_state = memory_state * decay_blk[:, None, None] + jnp.einsum('hcd,hce->hde', key_blk, new_values, precision=HIGHEST)
        return (memory_state, output)
    stacked = tuple((jnp.moveaxis(tensor, 1, 0) for tensor in (fresh_vals, correction, attend_map, query_dec, key_dec, carry_decay)))
    initial = jnp.zeros((heads_n, key_dim, values_in.shape[-1]), jnp.float32)
    _, outputs = lax.scan(advance, initial, stacked)
    return jnp.transpose(outputs, (1, 0, 2, 3)).reshape(heads_n, length, -1)

def mixer_output(query_raw, key_raw, value_raw, beta_raw, decay_raw, rate_vals):
    length = query_raw.shape[0]
    heads_n = beta_raw.shape[0]

    def heads_first(matrix):
        return jnp.transpose(matrix.astype(jnp.float32).reshape(length, heads_n, -1), (1, 0, 2))
    queries = heads_first(query_raw)
    keys_in = heads_first(key_raw)
    values_in = heads_first(value_raw)
    queries = queries * lax.rsqrt(lax.optimization_barrier(jnp.sum(queries * queries, axis=-1, keepdims=True)) + NORM_FLOOR) * queries.shape[-1] ** (-0.5)
    keys_in = keys_in * lax.rsqrt(lax.optimization_barrier(jnp.sum(keys_in * keys_in, axis=-1, keepdims=True)) + NORM_FLOOR)
    strength = jax.nn.sigmoid(beta_raw)
    log_decay = -rate_vals[:, None] * jax.nn.softplus(decay_raw)
    mixer_out = delta_mixer(queries, keys_in, values_in, strength, log_decay)
    return jnp.transpose(mixer_out, (1, 0, 2)).reshape(length, -1)

def request_slots(id_rows, pass_count):
    owners = id_rows // pass_count
    local_idx = id_rows % pass_count
    req_count = id_rows.shape[-1]
    req_order = jnp.arange(req_count, dtype=jnp.int32)
    earlier = (owners[..., :, None] == owners[..., None, :]) & (req_order[None, :] < req_order[:, None])
    ranks = lax.optimization_barrier(jnp.sum(earlier.astype(jnp.int32), axis=-1, dtype=jnp.int32))
    return (owners, local_idx, ranks)

def reference(tokens, cotangent, mix_query, mix_key, mix_value, beta_pre, decay_pre, decay_rate, passages, passage_ids, query_weight, key_weight, value_weight, gate_weight):
    score_scale = SCORE_GAIN * HEAD ** (-0.5)
    every_id = passage_ids.reshape(N_ST, REQ_DEV)
    query_heads = query_weight.astype(jnp.float32).reshape(D, HEADS, HEAD)
    key_heads = key_weight.astype(jnp.float32).reshape(D, HEADS, HEAD)
    value_heads = value_weight.astype(jnp.float32).reshape(D, HEADS, HEAD)
    gate_float = gate_weight.astype(jnp.float32)
    blocks_n = TOK_DEV // BLOCK

    def reader(reader_idx):
        first_row = reader_idx * TOK_DEV
        tok_block = lax.dynamic_slice_in_dim(tokens, first_row, TOK_DEV, 0)
        query_low = to_low(jnp.dot(tok_block, query_weight, preferred_element_type=jnp.float32))
        query_float = query_low.astype(jnp.float32).reshape(TOK_DEV, HEADS, HEAD)
        query_scale = lax.rsqrt(lax.optimization_barrier(jnp.mean(query_float * query_float, axis=-1, keepdims=True)) + NORM_FLOOR)
        query_hat = to_low(query_float * query_scale)
        gate_open = jax.nn.sigmoid(jnp.dot(tok_block, gate_weight.T, preferred_element_type=jnp.float32))
        row_block = passages[every_id[reader_idx]].reshape(REQ_DEV * PROWS, D)
        key_low = to_low(jnp.dot(row_block, key_weight, preferred_element_type=jnp.float32))
        key_float = key_low.astype(jnp.float32).reshape(REQ_DEV * PROWS, HEADS, HEAD)
        key_scale = lax.rsqrt(lax.optimization_barrier(jnp.mean(key_float * key_float, axis=-1, keepdims=True)) + NORM_FLOOR)
        key_hat = to_low(key_float * key_scale)
        value_low = to_low(jnp.dot(row_block, value_weight, preferred_element_type=jnp.float32))
        key_blocks = key_hat.astype(jnp.float32).reshape(blocks_n, PER_BLOCK * PROWS, HEADS, HEAD)
        value_blocks = value_low.astype(jnp.float32).reshape(blocks_n, PER_BLOCK * PROWS, HEADS, HEAD)
        query_blocks = query_hat.astype(jnp.float32).reshape(blocks_n, BLOCK, HEADS, HEAD)
        scores = jnp.einsum('bihd,bjhd->bhij', query_blocks, key_blocks) * score_scale
        exp_scores = jnp.exp(scores)
        attn_probs = exp_scores / lax.optimization_barrier(jnp.sum(exp_scores, axis=-1, keepdims=True))
        probs_low = to_low(attn_probs).astype(jnp.float32)
        retrieved = jnp.einsum('bhij,bjhd->bihd', probs_low, value_blocks).reshape(TOK_DEV, HEADS, HEAD)
        mixer_out = mixer_output(lax.dynamic_slice_in_dim(mix_query, first_row, TOK_DEV, 0), lax.dynamic_slice_in_dim(mix_key, first_row, TOK_DEV, 0), lax.dynamic_slice_in_dim(mix_value, first_row, TOK_DEV, 0), lax.dynamic_slice_in_dim(beta_pre, first_row, TOK_DEV, 1), lax.dynamic_slice_in_dim(decay_pre, first_row, TOK_DEV, 1), decay_rate).reshape(TOK_DEV, HEADS, HEAD)
        grad_out = lax.dynamic_slice_in_dim(cotangent, first_row, TOK_DEV, 0).astype(jnp.float32).reshape(TOK_DEV, HEADS, HEAD)
        grad_ret = to_low(gate_open[..., None] * grad_out).astype(jnp.float32)
        gate_grad = lax.optimization_barrier(jnp.sum(grad_out * (retrieved - mixer_out), axis=-1)) * gate_open * (1.0 - gate_open)
        grad_blocks = grad_ret.reshape(blocks_n, BLOCK, HEADS, HEAD)
        grad_probs = jnp.einsum('bihd,bjhd->bhij', grad_blocks, value_blocks)
        score_grad = to_low(attn_probs * (grad_probs - lax.optimization_barrier(jnp.sum(grad_probs * attn_probs, axis=-1, keepdims=True)))).astype(jnp.float32)
        qhat_grad = score_scale * jnp.einsum('bhij,bjhd->bihd', score_grad, key_blocks).reshape(TOK_DEV, HEADS, HEAD)
        khat_grad = to_low(score_scale * jnp.einsum('bhij,bihd->bjhd', score_grad, query_blocks)).astype(jnp.float32).reshape(REQ_DEV, PROWS, HEADS, HEAD)
        value_grad = to_low(jnp.einsum('bhij,bihd->bjhd', probs_low, grad_blocks)).astype(jnp.float32).reshape(REQ_DEV, PROWS, HEADS, HEAD)
        query_grad = to_low(query_scale * qhat_grad - query_scale ** 3 * query_float * lax.optimization_barrier(jnp.mean(query_float * qhat_grad, axis=-1, keepdims=True))).astype(jnp.float32)
        partial_value = jnp.einsum('thd,ehd->the', query_grad, query_heads) + gate_grad[..., None] * gate_float[None]
        token_rows = lax.optimization_barrier(jnp.sum(to_low(partial_value).astype(jnp.float32), axis=1)).astype(jnp.bfloat16)
        return (token_rows, khat_grad, value_grad)
    token_rows, khat_all, value_all = lax.map(reader, jnp.arange(N_ST, dtype=jnp.int32))
    owner_all, local_all, rank_all = request_slots(every_id, PASS_DEV)
    cap_iota = jnp.arange(CAP, dtype=jnp.int32)
    req_iota = jnp.arange(REQ_DEV, dtype=jnp.int32)
    readers = jnp.arange(N_ST, dtype=jnp.int32)[:, None]
    pass_iota = jnp.arange(PASS_DEV, dtype=jnp.int32)

    def owner_step(weight_acc, owner_idx):
        wanted = (owner_all == owner_idx)[:, None, :] & (rank_all[:, None, :] == cap_iota[None, :, None])
        slot_used = jnp.any(wanted, axis=-1)
        slot_local = lax.optimization_barrier(jnp.sum(jnp.where(wanted, local_all[:, None, :], 0), axis=-1, dtype=jnp.int32))
        req_pick = lax.optimization_barrier(jnp.sum(jnp.where(wanted, req_iota[None, None, :], 0), axis=-1, dtype=jnp.int32))
        khat_slots = jnp.where(slot_used[:, :, None, None, None], khat_all[readers, req_pick], 0.0)
        value_slots = jnp.where(slot_used[:, :, None, None, None], value_all[readers, req_pick], 0.0)
        onehot = ((slot_local.reshape(-1)[None, :] == pass_iota[:, None]) & slot_used.reshape(-1)[None, :]).astype(jnp.float32)
        khat_pass = jnp.dot(onehot, khat_slots.reshape(N_ST * CAP, -1), precision=HIGHEST).reshape(PASS_DEV * PROWS, HEADS, HEAD)
        value_pass = jnp.dot(onehot, value_slots.reshape(N_ST * CAP, -1), precision=HIGHEST).reshape(PASS_DEV * PROWS, HEADS, HEAD)
        row_block = lax.dynamic_slice_in_dim(passages, owner_idx * PASS_DEV, PASS_DEV, 0).reshape(PASS_DEV * PROWS, D)
        key_low = to_low(jnp.dot(row_block, key_weight, preferred_element_type=jnp.float32))
        key_float = key_low.astype(jnp.float32).reshape(PASS_DEV * PROWS, HEADS, HEAD)
        key_scale = lax.rsqrt(lax.optimization_barrier(jnp.mean(key_float * key_float, axis=-1, keepdims=True)) + NORM_FLOOR)
        key_grad = to_low(key_scale * khat_pass - key_scale ** 3 * key_float * lax.optimization_barrier(jnp.mean(key_float * khat_pass, axis=-1, keepdims=True)))
        value_grad_low = to_low(value_pass)
        partial_value = jnp.einsum('rhd,ehd->rhe', key_grad.astype(jnp.float32), key_heads) + jnp.einsum('rhd,ehd->rhe', value_grad_low.astype(jnp.float32), value_heads)
        rows_grad = lax.optimization_barrier(jnp.sum(to_low(partial_value).astype(jnp.float32), axis=1)).astype(jnp.bfloat16).reshape(PASS_DEV, PROWS, D)
        weight_acc = weight_acc + jnp.dot(row_block.T, key_grad.reshape(PASS_DEV * PROWS, HEADS * HEAD), preferred_element_type=jnp.float32)
        return (weight_acc, rows_grad)
    weight_grad, store_grad = lax.scan(owner_step, jnp.zeros((D, HEADS * HEAD), jnp.float32), jnp.arange(N_ST, dtype=jnp.int32))
    return (token_rows.reshape(TOKENS, D), store_grad.reshape(PASSAGES, PROWS, D), weight_grad)
```

```python
import functools

import jax
import jax.numpy as jnp
from jax import lax
from jax.experimental import pallas as pl
from jax.experimental.pallas import tpu as pltpu
from jax.sharding import PartitionSpec as P

SPAN = 64


NORM_FLOOR = 1.0
SCORE_GAIN = 4.0
HIGHEST = lax.Precision.HIGHEST
CONTRACT_LAST = (((1,), (1,)), ((), ()))
CONTRACT_FIRST = (((0,), (0,)), ((), ()))

MESH = pl.DeviceIdType.MESH
VMEM_SPEC = pl.BlockSpec(memory_space=pltpu.VMEM)
DMA = pltpu.SemaphoreType.DMA
CHUNK = 256


def tp_places():
    place = lax.axis_index("tp")
    parity = lax.rem(place, 2)
    half = place // 2
    return place, parity, half, place + 1 - 2 * parity, lax.rem(place + 2, 4)


def st_peer(me, step, st_count):
    if st_count & (st_count - 1):
        return lax.rem(me + step, st_count)
    flips = st_count - step
    peer = me
    for bit in range(st_count.bit_length() - 1):
        if flips >> bit & 1:
            peer = peer + (1 << bit) * (1 - 2 * lax.rem(me // (1 << bit), 2))
    return peer


def meet(st_count, with_st, with_tp=True):
    barrier = pltpu.get_barrier_semaphore()
    _, _, _, partner, far = tp_places()
    for other in (partner, far) if with_tp else ():
        pl.semaphore_signal(barrier, inc=1, device_id={"tp": other}, device_id_type=MESH)
    total = 2 if with_tp else 0
    if with_st:
        me = lax.axis_index("st")
        for step in range(1, st_count):
            pl.semaphore_signal(
                barrier,
                inc=1,
                device_id={"st": st_peer(me, step, st_count)},
                device_id_type=MESH,
            )
        total += st_count - 1
    pl.semaphore_wait(barrier, total)


def scatter_sum(term, out_ref, chunks, first_send, first_recv, kept, second_send, second_recv, sems):
    _, parity, half, partner, far = tp_places()
    send_a, recv_a, send_b, recv_b = sems
    rows = out_ref.shape[0] // chunks

    def pair_copy(k, i):
        return pltpu.make_async_remote_copy(
            src_ref=first_send.at[k, i],
            dst_ref=first_recv.at[k, i],
            send_sem=send_a.at[k, i],
            recv_sem=recv_a.at[k, i],
            device_id={"tp": partner},
            device_id_type=MESH,
        )

    def far_copy(k):
        return pltpu.make_async_remote_copy(
            src_ref=second_send.at[k],
            dst_ref=second_recv.at[k],
            send_sem=send_b.at[k],
            recv_sem=recv_b.at[k],
            device_id={"tp": far},
            device_id_type=MESH,
        )

    def pass_on(k):
        pair_copy(k, 0).wait_recv()
        second_send[k] = (
            kept[k, 0].astype(jnp.float32) + first_recv[k, 0].astype(jnp.float32)
        ).astype(jnp.bfloat16)
        far_copy(k).start()

    for k in range(chunks):
        for i in range(2):
            column = 2 * (1 - half if i == 0 else half)
            first_send[k, i] = term(k, column + 1 - parity).astype(jnp.bfloat16)
            pair_copy(k, i).start()
            kept[k, i] = term(k, column + parity).astype(jnp.bfloat16)
            if i == 0 and k >= 1:
                pass_on(k - 1)
    pass_on(chunks - 1)
    for k in range(chunks):
        pair_copy(k, 1).wait_recv()
        far_copy(k).wait_recv()
        out_ref[pl.ds(k * rows, rows), :] = (
            kept[k, 1].astype(jnp.float32)
            + first_recv[k, 1].astype(jnp.float32)
            + second_recv[k].astype(jnp.float32)
        ).astype(out_ref.dtype)
    for k in range(chunks):
        pair_copy(k, 0).wait_send()
        pair_copy(k, 1).wait_send()
        far_copy(k).wait_send()


def scatter_scratch(chunks, rows, width):
    return [
        pltpu.VMEM((chunks, 2, rows, width), jnp.bfloat16),
        pltpu.VMEM((chunks, 2, rows, width), jnp.bfloat16),
        pltpu.VMEM((chunks, 2, rows, width), jnp.bfloat16),
        pltpu.VMEM((chunks, rows, width), jnp.bfloat16),
        pltpu.VMEM((chunks, rows, width), jnp.bfloat16),
        DMA((chunks, 2)),
        DMA((chunks, 2)),
        DMA((chunks,)),
        DMA((chunks,)),
    ]


def project_kernel(
    st_count,
    ids_ref,
    rows_hbm,
    kw_ref,
    vw_ref,
    ids_all_ref,
    key_ref,
    packed_ref,
    rows_ref,
    rows_sem,
    id_send,
    id_recv,
):
    me = lax.axis_index("st")
    head_dim = kw_ref.shape[1]
    chunks = rows_ref.shape[0] // CHUNK

    def rows_copy(k):
        here = pl.ds(k * CHUNK, CHUNK)
        return pltpu.make_async_copy(rows_hbm.at[here, :], rows_ref.at[here, :], rows_sem.at[k])

    for k in range(chunks):
        rows_copy(k).start()
    meet(st_count, True, False)

    def id_copy(step):
        return pltpu.make_async_remote_copy(
            src_ref=ids_ref,
            dst_ref=ids_all_ref.at[me],
            send_sem=id_send.at[step],
            recv_sem=id_recv.at[step],
            device_id={"st": st_peer(me, step, st_count)},
            device_id_type=MESH,
        )

    for step in range(1, st_count):
        id_copy(step).start()
    ids_all_ref[pl.ds(me, 1)] = ids_ref[...][None]

    for k in range(chunks):
        rows_copy(k).wait()
        here = pl.ds(k * CHUNK, CHUNK)
        block = rows_ref[here, :]
        key_low = jnp.dot(block, kw_ref[...], preferred_element_type=jnp.float32).astype(
            jnp.bfloat16
        )
        key_ref[here, :] = key_low
        key_float = key_low.astype(jnp.float32)
        scale = lax.rsqrt(jnp.mean(key_float * key_float, axis=-1, keepdims=True) + NORM_FLOOR)
        packed_ref[here, pl.ds(0, head_dim)] = (key_float * scale).astype(jnp.bfloat16)
        packed_ref[here, pl.ds(head_dim, head_dim)] = jnp.dot(
            block, vw_ref[...], preferred_element_type=jnp.float32
        ).astype(jnp.bfloat16)

    for step in range(1, st_count):
        id_copy(step).wait()


def project_call(st_count, ids_padded, flat_rows, key_weight, value_weight):
    head_dim = key_weight.shape[1]
    total_rows = flat_rows.shape[0]
    return pl.pallas_call(
        functools.partial(project_kernel, st_count),
        out_shape=(
            jax.ShapeDtypeStruct((st_count, *ids_padded.shape), jnp.int32),
            jax.ShapeDtypeStruct((total_rows, head_dim), jnp.bfloat16),
            jax.ShapeDtypeStruct((total_rows, 2 * head_dim), jnp.bfloat16),
        ),
        in_specs=[VMEM_SPEC, pl.BlockSpec(memory_space=pl.ANY), VMEM_SPEC, VMEM_SPEC],
        out_specs=(VMEM_SPEC,) * 3,
        scratch_shapes=[
            pltpu.VMEM(flat_rows.shape, jnp.bfloat16),
            DMA((total_rows // CHUNK,)),
            DMA((st_count,)),
            DMA((st_count,)),
        ],
        compiler_params=pltpu.CompilerParams(collective_id=0, has_side_effects=True),
        name="ids_project",
    )(ids_padded, flat_rows, key_weight, value_weight)


def settle_kernel(*refs):
    count = len(refs) // 2
    for source, target in zip(refs[:count], refs[count:]):
        target[...] = source[...]


def settle_call(*arrays):
    return pl.pallas_call(
        settle_kernel,
        out_shape=tuple(jax.ShapeDtypeStruct(x.shape, x.dtype) for x in arrays),
        in_specs=[VMEM_SPEC] * len(arrays),
        out_specs=(VMEM_SPEC,) * len(arrays),
        name="settle",
    )(*arrays)


def exact_dot(left, right, dims=(((1,), (0,)), ((), ()))):
    return lax.dot_general(
        left, right, dims, precision=HIGHEST, preferred_element_type=jnp.float32
    )


def mixer_span(queries, keys_in, values_in, strength, log_decay, state):
    span = queries.shape[0]
    row_at = lax.broadcasted_iota(jnp.int32, (span, span), 0)
    col_at = lax.broadcasted_iota(jnp.int32, (span, span), 1)
    inclusive = row_at >= col_at
    unit_eye = jnp.where(row_at == col_at, 1.0, 0.0)
    decay_row = jnp.sum(unit_eye * log_decay, axis=0, keepdims=True)
    cum_row = jnp.sum(jnp.where(row_at <= col_at, log_decay, 0.0), axis=0, keepdims=True)
    cum_col = jnp.sum(jnp.where(inclusive, decay_row, 0.0), axis=1, keepdims=True)
    total = jnp.sum(log_decay, axis=0, keepdims=True)
    decay_map = jnp.exp(jnp.where(inclusive, cum_col - cum_row, -1e30))
    queries = (
        queries
        * lax.rsqrt(jnp.sum(queries * queries, axis=-1, keepdims=True) + NORM_FLOOR)
        * queries.shape[-1] ** (-0.5)
    )
    keys_in = keys_in * lax.rsqrt(jnp.sum(keys_in * keys_in, axis=-1, keepdims=True) + NORM_FLOOR)
    power = jnp.where(
        row_at > col_at, strength * exact_dot(keys_in, keys_in, CONTRACT_LAST) * decay_map, 0.0
    )
    inverse = unit_eye - power
    for _ in range(span.bit_length() - 2):
        power = exact_dot(power, power)
        inverse = exact_dot(inverse, unit_eye + power)
    attend = exact_dot(queries, keys_in, CONTRACT_LAST) * decay_map
    fresh = exact_dot(inverse, values_in * strength)
    correction = exact_dot(inverse, keys_in * (strength * jnp.exp(cum_col)))
    new_values = fresh - exact_dot(correction, state)
    output = exact_dot(queries * jnp.exp(cum_col), state) + exact_dot(attend, new_values)
    state = state * jnp.exp(total) + exact_dot(
        keys_in * jnp.exp(total - cum_col), new_values, CONTRACT_FIRST
    )
    return output, state


def main_kernel(
    st_count,
    sizes,
    local_ref,
    slot_ref,
    request_ref,
    rate_ref,
    code_ref,
    own_ref,
    packed_ref,
    key_ref,
    cot_ref,
    mq_ref,
    mk_ref,
    mv_ref,
    beta_ref,
    decay_ref,
    qw_ref,
    gate_ref,
    kw_ref,
    vw_ref,
    rows_hbm,
    tok_out,
    out_ref,
    weight_ref,
    tok_ref,
    tok_send,
    tok_recv,
    gw_ref,
    turned,
    rows_ref,
    rows_sem,
    send_buf,
    arrived,
    reply_rows,
    reply_send,
    reply_recv,
    x_sems,
    query_low,
    query_hat,
    query_grad,
    gate_grad,
    gate_open,
    mixed,
    states,
    block_kv,
    key_grad,
    value_grad,
    weight_send,
    weight_recv,
    w_send,
    w_recv,
    *scratch,
):
    cap, per_block, tok_chunks, row_chunks = sizes
    me = lax.axis_index("st")
    slot_total, span_rows, _ = send_buf.shape
    head_dim = key_ref.shape[1]
    part = weight_ref.shape[0]
    blocks_n = slot_ref.shape[0] // per_block
    block_rows = tok_ref.shape[0] // blocks_n
    heads_n = beta_ref.shape[0]
    mix_dim = mq_ref.shape[1] // heads_n
    score_scale = SCORE_GAIN * head_dim ** (-0.5)
    rows_copy = pltpu.make_async_copy(rows_hbm, rows_ref, rows_sem)
    rows_copy.start()
    meet(st_count, True)

    def exchange(lane, source, target, step):
        peer = st_peer(me, step, st_count)
        return pltpu.make_async_remote_copy(
            src_ref=source.at[pl.ds(peer * cap, cap)],
            dst_ref=target.at[pl.ds(me * cap, cap)],
            send_sem=x_sems.at[lane, 0, step],
            recv_sem=x_sems.at[lane, 1, step],
            device_id={"st": peer},
            device_id_type=MESH,
        )

    place, _, _, partner, far = tp_places()
    own_width = own_ref.shape[1]

    def tok_columns(which):
        return pl.ds(pl.multiple_of(which * own_width, own_width), own_width)

    def tok_copy(lane, source, which, target):
        return pltpu.make_async_remote_copy(
            src_ref=source,
            dst_ref=tok_ref.at[:, tok_columns(which)],
            send_sem=tok_send.at[lane],
            recv_sem=tok_recv.at[lane],
            device_id={"tp": target},
            device_id_type=MESH,
        )

    to_partner = tok_copy(0, own_ref, place, partner)
    to_far = tok_copy(1, own_ref, place, far)
    onward = tok_copy(2, tok_ref.at[:, tok_columns(far)], far, partner)
    to_far.start()
    for step in range(1, st_count):
        peer = st_peer(me, step, st_count)
        for c in range(cap):
            send_buf[peer * cap + c] = packed_ref[local_ref[peer * cap + c]]
        exchange(0, send_buf, arrived, step).start()
    for c in range(cap):
        arrived[me * cap + c] = packed_ref[local_ref[me * cap + c]]

    to_partner.start()
    tok_ref[:, tok_columns(place)] = own_ref[...]
    gw_ref[...] = gate_ref[...].astype(jnp.float32)
    turned[...] = jnp.transpose(
        jnp.concatenate(
            [
                beta_ref[...],
                decay_ref[...],
                jnp.zeros((8 - 2 * heads_n, beta_ref.shape[1]), jnp.float32),
            ],
            axis=0,
        )
    )
    states[...] = jnp.zeros_like(states)

    def mix(b):
        here = pl.ds(pl.multiple_of(b * SPAN, SPAN), SPAN)
        for m in range(heads_n):
            cols = pl.ds(m * mix_dim, mix_dim)
            raw = turned[here, heads_n + m : heads_n + m + 1]
            softplus = jnp.maximum(raw, 0.0) + jnp.log1p(jnp.exp(-jnp.abs(raw)))
            mixed[here, cols], states[m] = mixer_span(
                mq_ref[here, cols].astype(jnp.float32),
                mk_ref[here, cols].astype(jnp.float32),
                mv_ref[here, cols].astype(jnp.float32),
                jax.nn.sigmoid(turned[here, m : m + 1]),
                -rate_ref[m] * softplus,
                states[m],
            )

    spans_n = tok_ref.shape[0] // SPAN
    pl.loop(0, spans_n // 2)(mix)
    to_far.wait_recv()
    onward.start()
    pl.loop(spans_n // 2, spans_n)(mix)
    to_partner.wait_recv()
    onward.wait_recv()

    @pl.loop(0, blocks_n)
    def _(b):
        here = pl.ds(pl.multiple_of(b * block_rows, block_rows), block_rows)
        low = jnp.dot(tok_ref[here, :], qw_ref[...], preferred_element_type=jnp.float32).astype(
            jnp.bfloat16
        )
        query_low[here, :] = low
        low = low.astype(jnp.float32)
        scale = lax.rsqrt(jnp.mean(low * low, axis=-1, keepdims=True) + NORM_FLOOR)
        query_hat[here, :] = (low * scale).astype(jnp.bfloat16)
        gate_open[here, :] = jax.nn.sigmoid(
            jnp.sum(tok_ref[here, :].astype(jnp.float32) * gw_ref[...], axis=-1, keepdims=True)
        )

    for step in range(1, st_count):
        exchange(0, send_buf, arrived, step).wait_recv()

    @pl.loop(0, blocks_n)
    def _(b):
        here = pl.ds(pl.multiple_of(b * block_rows, block_rows), block_rows)
        for j in range(per_block):
            block_kv[pl.ds(j * span_rows, span_rows), :] = arrived[slot_ref[b * per_block + j]]
        keys = block_kv[:, :head_dim]
        values = block_kv[:, head_dim:]
        q_hat = query_hat[here, :]
        opened = gate_open[here, :]
        cot = cot_ref[here, :].astype(jnp.float32)
        grad_ret = (opened * cot).astype(jnp.bfloat16)
        exp_scores = jnp.exp(
            lax.dot_general(q_hat, keys, CONTRACT_LAST, preferred_element_type=jnp.float32)
            * score_scale
        )
        probs = exp_scores / jnp.sum(exp_scores, axis=-1, keepdims=True)
        probs_low = probs.astype(jnp.bfloat16)
        retrieved = jnp.dot(probs_low, values, preferred_element_type=jnp.float32)
        gate_grad[here, :] = (
            jnp.sum(cot * (retrieved - mixed[here, :]), axis=-1, keepdims=True)
            * opened
            * (1.0 - opened)
        )
        grad_probs = lax.dot_general(
            grad_ret, values, CONTRACT_LAST, preferred_element_type=jnp.float32
        )
        score_grad = (
            probs * (grad_probs - jnp.sum(grad_probs * probs, axis=-1, keepdims=True))
        ).astype(jnp.bfloat16)
        key_term = (
            score_scale
            * lax.dot_general(score_grad, q_hat, CONTRACT_FIRST, preferred_element_type=jnp.float32)
        ).astype(jnp.bfloat16)
        value_term = lax.dot_general(
            probs_low, grad_ret, CONTRACT_FIRST, preferred_element_type=jnp.float32
        ).astype(jnp.bfloat16)
        for j in range(per_block):
            piece = slice(j * span_rows, (j + 1) * span_rows)
            reply_rows[b * per_block + j, :, pl.ds(0, head_dim)] = key_term[piece]
            reply_rows[b * per_block + j, :, pl.ds(head_dim, head_dim)] = value_term[piece]
        hat_grad = score_scale * jnp.dot(score_grad, keys, preferred_element_type=jnp.float32)
        low = query_low[here, :].astype(jnp.float32)
        scale = lax.rsqrt(jnp.mean(low * low, axis=-1, keepdims=True) + NORM_FLOOR)
        query_grad[here, :] = (
            scale * hat_grad
            - scale * scale * scale * low * jnp.mean(low * hat_grad, axis=-1, keepdims=True)
        ).astype(jnp.bfloat16)

    for step in range(1, st_count):
        peer = st_peer(me, step, st_count)
        for c in range(cap):
            reply_send[peer * cap + c] = reply_rows[request_ref[peer * cap + c]]
        exchange(1, reply_send, reply_recv, step).start()
    for c in range(cap):
        reply_recv[me * cap + c] = reply_rows[request_ref[me * cap + c]]

    tok_width = tok_out.shape[1]
    tok_rows = tok_out.shape[0] // tok_chunks

    def token_term(k, which):
        here = pl.ds(k * tok_rows, tok_rows)
        cols = pl.ds(pl.multiple_of(which * tok_width, tok_width), tok_width)
        return (
            lax.dot_general(
                query_grad[here, :],
                qw_ref[cols, :],
                CONTRACT_LAST,
                preferred_element_type=jnp.float32,
            )
            + gate_grad[here, :] * gw_ref[:, cols]
        )

    scatter_sum(token_term, tok_out, tok_chunks, *scratch[:5], scratch[5:9])

    for step in range(1, st_count):
        exchange(1, reply_send, reply_recv, step).wait_recv()

    @pl.loop(0, out_ref.shape[0] // CHUNK)
    def _(k):
        here = pl.ds(pl.multiple_of(k * CHUNK, CHUNK), CHUNK)
        row_at = lax.broadcasted_iota(jnp.int32, (CHUNK, code_ref.shape[1]), 0) + k * CHUNK
        pick = jnp.where(row_at == code_ref[...], 1.0, 0.0).astype(jnp.bfloat16)
        summed = jnp.dot(
            pick,
            reply_recv[...].reshape(slot_total * span_rows, 2 * head_dim),
            preferred_element_type=jnp.float32,
        )
        hat_grad = summed[:, :head_dim]
        key_float = key_ref[here, :].astype(jnp.float32)
        scale = lax.rsqrt(jnp.mean(key_float * key_float, axis=-1, keepdims=True) + NORM_FLOOR)
        key_grad[here, :] = (
            scale * hat_grad
            - scale * scale * scale
            * key_float
            * jnp.mean(key_float * hat_grad, axis=-1, keepdims=True)
        ).astype(jnp.bfloat16)
        value_grad[here, :] = summed[:, head_dim:].astype(jnp.bfloat16)

    rows_copy.wait()

    def own_part(which):
        return weight_send.at[pl.ds(pl.multiple_of(which * part, part), part), :]

    def weight_copy(step):
        target = st_peer(me, step, st_count)
        return pltpu.make_async_remote_copy(
            src_ref=own_part(target),
            dst_ref=weight_recv.at[step],
            send_sem=w_send.at[step],
            recv_sem=w_recv.at[step],
            device_id={"st": target},
            device_id_type=MESH,
        )

    @pl.loop(0, weight_send.shape[0] // CHUNK)
    def _(k):
        here = pl.ds(pl.multiple_of(k * CHUNK, CHUNK), CHUNK)
        weight_send[here, :] = lax.dot_general(
            rows_ref[:, here], key_grad[...], CONTRACT_FIRST, preferred_element_type=jnp.float32
        ).astype(jnp.bfloat16)

    for step in range(1, st_count):
        weight_copy(step).start()

    width = out_ref.shape[1]
    rows = out_ref.shape[0] // row_chunks

    def row_term(k, which):
        here = pl.ds(k * rows, rows)
        cols = pl.ds(pl.multiple_of(which * width, width), width)
        return lax.dot_general(
            key_grad[here, :], kw_ref[cols, :], CONTRACT_LAST, preferred_element_type=jnp.float32
        ) + lax.dot_general(
            value_grad[here, :], vw_ref[cols, :], CONTRACT_LAST, preferred_element_type=jnp.float32
        )

    scatter_sum(row_term, out_ref, row_chunks, *scratch[9:14], scratch[14:18])
    weight_ref[...] = own_part(me)[...].astype(jnp.float32)
    for step in range(1, st_count):
        weight_copy(step).wait_recv()
        weight_ref[...] += weight_recv[step].astype(jnp.float32)
    for step in range(1, st_count):
        weight_copy(step).wait_send()
        exchange(0, send_buf, arrived, step).wait_send()
        exchange(1, reply_send, reply_recv, step).wait_send()
    to_partner.wait_send()
    to_far.wait_send()
    onward.wait_send()


def main_call(st_count, cap, per_block, span_rows, *operands):
    slot_local, tok, key_low, cot = operands[0], operands[5], operands[7], operands[8]
    flat_rows = operands[-1]
    heads_n = operands[12].shape[0]
    slot_total = slot_local.shape[0]
    tok_rows, model_width = tok.shape[0], flat_rows.shape[1]
    rows, head_dim = key_low.shape
    width = model_width // 4
    part = model_width // st_count
    tok_chunks, row_chunks = 3, 4
    mix_dim = cot.shape[1] // heads_n
    slots = pltpu.VMEM((slot_total, span_rows, 2 * head_dim), jnp.bfloat16)
    smem = pl.BlockSpec(memory_space=pltpu.SMEM)
    return pl.pallas_call(
        functools.partial(main_kernel, st_count, (cap, per_block, tok_chunks, row_chunks)),
        out_shape=(
            jax.ShapeDtypeStruct((tok_rows, width), jnp.bfloat16),
            jax.ShapeDtypeStruct((rows, width), jnp.bfloat16),
            jax.ShapeDtypeStruct((part, head_dim), jnp.float32),
        ),
        in_specs=[smem] * 4 + [VMEM_SPEC] * 14 + [pl.BlockSpec(memory_space=pl.ANY)],
        out_specs=(VMEM_SPEC,) * 3,
        scratch_shapes=[
            pltpu.VMEM((tok_rows, model_width), jnp.bfloat16),
            DMA((3,)),
            DMA((3,)),
            pltpu.VMEM((1, model_width), jnp.float32),
            pltpu.VMEM((tok_rows, 8), jnp.float32),
            pltpu.VMEM(flat_rows.shape, jnp.bfloat16),
            DMA(()),
            slots,
            slots,
            pltpu.VMEM((operands[1].shape[0], span_rows, 2 * head_dim), jnp.bfloat16),
            slots,
            slots,
            DMA((2, 2, st_count)),
            pltpu.VMEM((tok_rows, head_dim), jnp.bfloat16),
            pltpu.VMEM((tok_rows, head_dim), jnp.bfloat16),
            pltpu.VMEM((tok_rows, head_dim), jnp.bfloat16),
            pltpu.VMEM((tok_rows, 1), jnp.float32),
            pltpu.VMEM((tok_rows, 1), jnp.float32),
            pltpu.VMEM((tok_rows, head_dim), jnp.float32),
            pltpu.VMEM((heads_n, mix_dim, mix_dim), jnp.float32),
            pltpu.VMEM((per_block * span_rows, 2 * head_dim), jnp.bfloat16),
            pltpu.VMEM((rows, head_dim), jnp.bfloat16),
            pltpu.VMEM((rows, head_dim), jnp.bfloat16),
            pltpu.VMEM((model_width, head_dim), jnp.bfloat16),
            pltpu.VMEM((st_count, part, head_dim), jnp.bfloat16),
            DMA((st_count,)),
            DMA((st_count,)),
            *scatter_scratch(tok_chunks, tok_rows // tok_chunks, width),
            *scatter_scratch(row_chunks, rows // row_chunks, width),
        ],
        compiler_params=pltpu.CompilerParams(collective_id=1, has_side_effects=True),
        name="exchange_attend",
    )(*operands)


def request_slots(id_rows, pass_count):
    owners = id_rows // pass_count
    local_idx = id_rows % pass_count
    req_count = id_rows.shape[-1]
    req_order = jnp.arange(req_count, dtype=jnp.int32)
    earlier = (owners[..., :, None] == owners[..., None, :]) & (
        req_order[None, :] < req_order[:, None]
    )
    ranks = jnp.sum(earlier.astype(jnp.int32), axis=-1, dtype=jnp.int32)
    return (owners, local_idx, ranks)


def body(
    tokens,
    cotangent,
    mix_query,
    mix_key,
    mix_value,
    beta_pre,
    decay_pre,
    decay_rate,
    passages,
    passage_ids,
    query_weight,
    key_weight,
    value_weight,
    gate_weight,
):
    model_width = query_weight.shape[0]
    head_dim = query_weight.shape[1]
    pass_local = passages.shape[0]
    span_rows = passages.shape[1]
    blocks_n = passage_ids.shape[0]
    per_block = passage_ids.shape[1]
    req_count = blocks_n * per_block
    st_count = lax.axis_size("st")
    my_owner = lax.axis_index("st")
    cap_count = max(1, req_count // st_count)
    slot_total = st_count * cap_count
    req_order = jnp.arange(req_count, dtype=jnp.int32)
    flat_rows = passages.reshape(pass_local * span_rows, model_width)
    flat_ids = passage_ids.reshape(1, req_count)
    ids_padded = jnp.pad(flat_ids, ((0, 7), (0, -req_count % 128)))
    ids_all, key_low, packed = project_call(
        st_count, ids_padded, flat_rows, key_weight, value_weight
    )
    every_id = ids_all[:, 0, :req_count]
    packed = packed.reshape(pass_local, span_rows, 2 * head_dim)
    all_owner, all_local, all_rank = request_slots(every_id, pass_local)
    cap_iota = jnp.arange(cap_count, dtype=jnp.int32)
    wanted = (all_owner == my_owner)[:, None, :] & (all_rank[:, None, :] == cap_iota[None, :, None])
    slot_used = jnp.any(wanted, axis=-1)
    slot_local = jnp.sum(jnp.where(wanted, all_local[:, None, :], 0), axis=-1, dtype=jnp.int32)
    own_owner, _, own_rank = request_slots(passage_ids.reshape(req_count), pass_local)
    slot_of = own_owner * cap_count + own_rank
    slot_match = slot_of[None, :] == jnp.arange(slot_total, dtype=jnp.int32)[:, None]
    slot_req = jnp.sum(jnp.where(slot_match, req_order[None, :], 0), axis=-1, dtype=jnp.int32)
    slot_row = jnp.where(slot_used, slot_local * span_rows, -span_rows).reshape(slot_total, 1)
    code = (slot_row + jnp.arange(span_rows, dtype=jnp.int32)[None, :]).reshape(1, -1)
    token_grad, passage_grad, key_weight_grad = main_call(
        st_count,
        cap_count,
        per_block,
        span_rows,
        slot_local.reshape(slot_total),
        slot_of,
        slot_req,
        decay_rate,
        code,
        tokens,
        packed,
        key_low,
        cotangent,
        mix_query,
        mix_key,
        mix_value,
        beta_pre,
        decay_pre,
        query_weight,
        gate_weight,
        key_weight,
        value_weight,
        flat_rows,
    )
    token_grad, passage_grad, key_weight_grad = settle_call(
        token_grad, passage_grad, key_weight_grad
    )
    passage_grad = passage_grad.reshape(pass_local, span_rows, -1)
    return (token_grad, passage_grad, key_weight_grad)


def solution(mesh):
    placed = (
        P("st", "tp"),
        P("st", "tp"),
        P("st", "tp"),
        P("st", "tp"),
        P("st", "tp"),
        P("tp", "st"),
        P("tp", "st"),
        P("tp"),
        P("st", None, None),
        P("st", None),
        P(None, "tp"),
        P(None, "tp"),
        P(None, "tp"),
        P("tp", None),
    )
    return jax.shard_map(
        body,
        mesh=mesh,
        in_specs=placed,
        out_specs=(P("st", "tp"), P("st", None, "tp"), P("st", "tp")),
        check_vma=False,
    )
```
